32 devices in a mesh: ep: 16 (over z, y, x), tp: 2 (over core).
Axes of the slice: x: 2, y: 2, z: 4, core: 2. Of those that a mesh axis runs over, the one named last changes fastest.
Arguments:
- inputs: bfloat16 [8192, 2048], P(('ep', 'tp')), may hold values from -6 to 6
- pre_gain: float32 [2048], replicated, may hold values from 0.5 to 8
- expert_ids: int32 [8192, 2], P(('ep', 'tp')), may hold values from 0 to 15, all different within a row; in each aligned block of 256 rows (0 to 255, 256 to 511, ...) at most 48 rows name the same one
- route_weights: float32 [8192, 2], P(('ep', 'tp')), may hold values from 0.05 to 1
- gate_proj: bfloat16 [16, 2048, 2048], P('ep', None, 'tp'), may hold values from -0.125 to 0.125
- up_proj: bfloat16 [16, 2048, 2048], P('ep', None, 'tp'), may hold values from -0.125 to 0.125
- down_proj: bfloat16 [16, 2048, 2048], P('ep', 'tp'), may hold values from -0.125 to 0.125
- post_gain: float32 [2048], replicated, may hold values from 0.1 to 1.9
Outputs:
- layer_out: bfloat16 [8192, 2048], P(('ep', 'tp'))
The draws below stay inside these ranges and needn't reach their ends.
Inputs may be any that keep to these rules, and one draw needn't show every extreme that they name: `expert_ids`: each token names 2 different experts. Among the 256 tokens of one device (aligned blocks of rows) no expert is named by more than 48 tokens, and in every draw some expert is named by exactly 48 tokens of some device.
All inputs are finite; a program needn't handle non-finite values.
Results may differ from the reference program's by a relative error of at most 0.0095.
Values may be sent and summed in bfloat16 or wider, within the bound.
A program may use at most 128 MiB of HBM per device.

```python
import math
import jax
import jax.numpy as jnp
import numpy as np
from jax import lax

D = 2048
FE = 2048
TOP_K = 2
TOK_DEV = 256
EXPERTS = 16
CAP = 48
TOKENS = 8192
N_EP = 16
N_TP = 2


def draw_pre_gain(key, part):
    return 1.0 + 0.18 * jnp.clip(jax.random.normal(key, (D,), jnp.float32), -2.5, 2.5)


def level_of(rng, dims, split, low, high):
    loudness = 1.0
    for dim, shards_of in split:
        steps = jax.random.uniform(jax.random.fold_in(jax.random.fold_in(rng, 6), dim), (shards_of,), jnp.float32, low / len(split), high / len(split))
        loudness = loudness * jnp.repeat(jnp.exp(steps), dims[dim] // shards_of).reshape((-1,) + (1,) * (len(dims) - 1 - dim))
    return loudness


def shared_out(stream_key, own, number, rows, count, top, reach, skew):
    sequence = jax.random.permutation(stream_key, count)
    packed, ordinary = shares(count, rows * top, reach, skew, True), shares(count, rows * top, reach, skew, False)
    places = jnp.arange(count)

    def named(tallies, turn):
        used = int((tallies > 0).sum())
        fixed = max(1, used // 4)
        moved = fixed + (places - fixed + turn * (used - fixed)) % max(1, count - fixed)
        return jnp.zeros((count,), jnp.int32).at[sequence[jnp.where(places < fixed, places, moved)]].set(jnp.asarray(tallies, jnp.int32))

    tallies = jnp.where(number % 4 == 0, named(packed, number // 4), named(ordinary, number - number // 4 - 1))
    mixed = jax.random.permutation(jax.random.fold_in(own, 3), count)
    giver, taker = mixed[0:count // 2 * 2:2], mixed[1:count // 2 * 2:2]
    margin = jnp.minimum(tallies[giver] - 1, reach - tallies[taker]) // 2
    margin = jnp.where((giver == sequence[0]) | (taker == sequence[0]) | (tallies[taker] == 0), 0, jnp.maximum(margin, 0))
    moved = jax.random.randint(jax.random.fold_in(own, 4), (count // 2,), 0, 1 << 20) % (margin + 1)
    tallies = tallies.at[giver].add(-moved).at[taker].add(moved)
    items = jnp.searchsorted(jnp.cumsum(tallies), jnp.arange(rows * top), side="right").astype(jnp.int32)
    listing = items.reshape(top, rows).T
    listing = listing[jax.random.permutation(jax.random.fold_in(own, 1), rows)]
    turn = jax.random.randint(jax.random.fold_in(own, 2), (rows, 1), 0, top)
    return jnp.take_along_axis(listing, (jnp.arange(top)[None, :] + turn) % top, axis=1)


def shares(amount, total, reach, lean, full):
    portions = [(1 << 20) // math.isqrt(standing ** lean) + 1 for standing in range(1, amount + 1)]
    largest = reach if full else min(reach, max(-(-total // amount), total * portions[0] // sum(portions)))
    least = 1 if total - largest >= amount - 1 else 0
    holding, surplus = [largest] + [least] * (amount - 1), total - largest - least * (amount - 1)
    while surplus > 0:
        movable = [i for i in range(1, amount) if holding[i] < largest] or [i for i in range(1, amount) if holding[i] < reach]
        whole, left = sum([portions[i] for i in movable]), surplus
        for i in movable:
            extra = min(reach - holding[i], max(1, left * portions[i] // whole), surplus)
            holding[i] = holding[i] + extra
            surplus = surplus - extra
    return np.array(holding)


def gaussian(key, shape, scale, most, shards=(), held_as=jnp.bfloat16):
    drawn = jax.random.normal(key, shape, jnp.float32) * scale
    if len(shards) > 0:
        drawn = level_of(key, shape, shards, -0.22, 0.18) * drawn
    return jnp.clip(drawn, min=-most, max=most).astype(held_as)


def setup_inputs(seed: int = 0) -> dict:
    keys = jax.random.split(jax.random.key(seed), 9)
    inputs = gaussian(keys[0], (TOKENS, D), 1.0, 6.0, ((0, 32),))
    pre_gain = draw_pre_gain(jax.random.fold_in(keys[8], 71), 0)
    expert_ids_keys = jax.random.split(jax.random.fold_in(keys[2], 1), TOKENS // TOK_DEV)
    expert_ids_turns = jax.random.permutation(jax.random.fold_in(keys[2], 3), TOKENS // TOK_DEV)
    expert_ids = jax.vmap(lambda own, number: shared_out(jax.random.fold_in(keys[2], 2), own, number, TOK_DEV, EXPERTS, TOP_K, CAP, 2))(expert_ids_keys, expert_ids_turns).reshape((TOKENS, TOP_K))
    route_weights = jnp.clip(jnp.exp(math.log(1.0) - 2.9957323 * jax.random.uniform(keys[3], (TOKENS, TOP_K), jnp.float32) ** level_of(keys[3], (TOKENS, TOP_K), ((0, 32),), -0.2, 0.2)), 0.05, 1.0)
    gate_proj = gaussian(keys[4], (EXPERTS, D, FE), D ** -0.5, 0.125, ((0, 16), (2, 2)))
    up_proj = gaussian(keys[5], (EXPERTS, D, FE), D ** -0.5, 0.125, ((0, 16), (2, 2)))
    down_proj = gaussian(keys[6], (EXPERTS, FE, D), FE ** -0.5, 0.125, ((0, 16), (1, 2)))
    post_gain = jnp.clip(1.0 + 0.18 * jax.random.normal(keys[7], (D,), jnp.float32), 0.1, 1.9)
    return {"inputs": inputs, "pre_gain": pre_gain, "expert_ids": expert_ids, "route_weights": route_weights, "gate_proj": gate_proj, "up_proj": up_proj, "down_proj": down_proj, "post_gain": post_gain}


EPSILON = 1e-06
LIMIT = 7.0
ALPHA = 1.702

def norm_rows(values, gain):
    floats = values.astype(jnp.float32)
    return floats * lax.rsqrt(lax.optimization_barrier(jnp.mean(floats * floats, axis=-1, keepdims=True)) + EPSILON) * gain

def activate(gate, up):
    gate = jnp.minimum(gate, LIMIT)
    up = jnp.clip(up, -LIMIT, LIMIT)
    return ((up + 1.0) * gate * jax.nn.sigmoid(ALPHA * gate)).astype(jnp.bfloat16)

def reference(inputs, pre_gain, expert_ids, route_weights, gate_proj, up_proj, down_proj, post_gain):
    devices_all = N_EP * N_TP
    normed = norm_rows(inputs, pre_gain).astype(jnp.bfloat16)
    blocks = expert_ids.reshape(devices_all, TOK_DEV * TOP_K)
    one_hot = (blocks[:, :, None] == jnp.arange(EXPERTS, dtype=jnp.int32)[None, None, :]).astype(jnp.int32)
    earlier = jnp.cumsum(one_hot, axis=1) - one_hot
    slot = lax.optimization_barrier(jnp.sum(earlier * one_hot, axis=-1))
    source = jnp.arange(devices_all, dtype=jnp.int32)[:, None]
    target = (blocks * (devices_all * CAP) + source * CAP + slot).reshape(-1).astype(jnp.int32)
    copies = jnp.repeat(normed, TOP_K, axis=0)
    buffer = jnp.zeros((EXPERTS * devices_all * CAP, D), jnp.bfloat16).at[target].set(copies)
    buffer = buffer.reshape(EXPERTS, devices_all * CAP, D)
    half = FE // N_TP

    def one_expert(operands):
        rows, w_gate, w_up, w_down = operands
        gate = jnp.dot(rows, w_gate, preferred_element_type=jnp.float32)
        up = jnp.dot(rows, w_up, preferred_element_type=jnp.float32)
        hidden = activate(gate, up)
        total = jnp.zeros((rows.shape[0], D), jnp.float32)
        for index in range(N_TP):
            part = jnp.dot(hidden[:, index * half:(index + 1) * half], w_down[index * half:(index + 1) * half], preferred_element_type=jnp.float32)
            part = lax.optimization_barrier(part.astype(jnp.bfloat16))
            total = total + part.astype(jnp.float32)
        return total.astype(jnp.bfloat16)
    results = lax.map(one_expert, (buffer, gate_proj, up_proj, down_proj)).reshape(-1, D)
    picked = results[target].reshape(TOKENS, TOP_K, D).astype(jnp.float32)
    mixed = lax.optimization_barrier(jnp.sum(picked * route_weights[:, :, None], axis=1))
    return norm_rows(mixed, post_gain).astype(jnp.bfloat16)
```

```python
import functools

import jax
import jax.numpy as jnp
from jax import lax
from jax.experimental import pallas as pl
from jax.experimental.pallas import tpu as pltpu
from jax.sharding import PartitionSpec as P

EPSILON = 1e-06
LIMIT = 7.0
ALPHA = 1.702
CHUNKS = 4
TILE = 256
MESH = pl.DeviceIdType.MESH


def activate(gate, up):
    gate = jnp.minimum(gate, LIMIT)
    up = jnp.clip(up, -LIMIT, LIMIT)
    return ((up + 1.0) * gate * jax.nn.sigmoid(ALPHA * gate)).astype(jnp.bfloat16)


def dot(a, b):
    return jnp.dot(a, b, preferred_element_type=jnp.float32)


def kernel(
    n, tps, cap,
    x_ref, pre_ref, meta_ref, gate_ref, up_ref, down_ref, post_ref, out_ref,
    gate_v, up_v, down_v, normed, prox, pmeta, send, recv, res, ret, part_send, part_recv,
    mixed, hidden, places,
    w_local, w_send, w_recv, p_send, p_recv, m_send, m_recv,
    d_send, d_recv, r_send, r_recv, q_send, q_recv,
):
    half = n // 2
    tokens, width = x_ref.shape
    cw = width // CHUNKS
    rows = half * cap
    fh = gate_v.shape[2]
    me = lax.axis_index("ep")
    core = lax.axis_index("tp")
    base = (me // half) * half
    mine = lax.rem(me, half)
    proxy = lax.rem(me + half, n)

    def member(j):
        return base + lax.rem(mine + j, half)

    barrier = pltpu.get_barrier_semaphore()

    @pl.loop(1, half)
    def _(j):
        pl.semaphore_signal(barrier, inc=1, device_id={"ep": member(j)}, device_id_type=MESH)

    pl.semaphore_signal(barrier, inc=1, device_id={"ep": proxy}, device_id_type=MESH)
    for i in range(1, tps):
        pl.semaphore_signal(
            barrier, inc=1, device_id={"tp": lax.rem(core + i, tps)}, device_id_type=MESH
        )
    pl.semaphore_wait(barrier, half + tps - 1)

    def remote(src, dst, ss, rs, where):
        return pltpu.make_async_remote_copy(
            src_ref=src, dst_ref=dst, send_sem=ss, recv_sem=rs,
            device_id=where, device_id_type=MESH,
        )

    def await_bytes(ref, sem):
        pltpu.make_async_copy(ref, ref, sem).wait()

    remote(meta_ref, pmeta, m_send, m_recv, {"ep": proxy}).start()
    weights = ((gate_ref, gate_v), (up_ref, up_v), (down_ref, down_v))
    local_copies, peer_copies = [], []
    for w, (src, dst) in enumerate(weights):
        local_copies.append(pltpu.make_async_copy(src.at[0], dst.at[core], w_local.at[w]))
        for i in range(1, tps):
            peer_copies.append(
                remote(
                    src.at[0], dst.at[core], w_send.at[w, i - 1], w_recv.at[w, i - 1],
                    {"tp": lax.rem(core + i, tps)},
                )
            )
    for copy in peer_copies + local_copies:
        copy.start()

    experts_col = lax.broadcasted_iota(jnp.int32, (n, 1), 0).astype(jnp.float32)
    earlier_mask = (
        lax.broadcasted_iota(jnp.int32, (tokens, tokens), 0)
        < lax.broadcasted_iota(jnp.int32, (tokens, tokens), 1)
    ).astype(jnp.bfloat16)

    def place(k, meta):
        first, second = meta[0:1, :], meta[1:2, :]
        hot0 = (first == experts_col).astype(jnp.float32)
        hot1 = (second == experts_col).astype(jnp.float32)
        before = dot((hot0 + hot1).astype(jnp.bfloat16), earlier_mask)
        places[k] = meta
        for i, (ids, hot) in enumerate(((first, hot0), (second, hot1))):
            slot = jnp.sum(before * hot, axis=0, keepdims=True)
            relative = ids - (base + mine).astype(jnp.float32)
            inside = (ids >= base.astype(jnp.float32)) & (
                ids < (base + half).astype(jnp.float32)
            )
            relative = jnp.where(relative < 0, relative + half, relative)
            places[k, i : i + 1, :] = jnp.where(inside, relative * cap + slot, -1.0)

    def picker(k):
        at = lax.broadcasted_iota(jnp.int32, (rows, 1), 0).astype(jnp.float32)
        return (
            (places[k, 0:1, :] == at).astype(jnp.float32)
            + (places[k, 1:2, :] == at).astype(jnp.float32)
        ).astype(jnp.bfloat16)

    def mixer(k):
        columns = places[k].T
        at = lax.broadcasted_iota(jnp.int32, (1, rows), 1).astype(jnp.float32)
        w = jnp.where(columns[:, 0:1] == at, columns[:, 2:3], 0.0) + jnp.where(
            columns[:, 1:2] == at, columns[:, 3:4], 0.0
        )
        high = w.astype(jnp.bfloat16)
        return high, (w - high.astype(jnp.float32)).astype(jnp.bfloat16)

    def dispatch(k, c, values):
        picked = dot(picker(k), values).astype(jnp.bfloat16)
        recv[k, c, 0:cap, :] = picked[0:cap]
        send[k, c, cap:rows, :] = picked[cap:rows]

        @pl.loop(1, half)
        def _(j):
            block = pl.ds(pl.multiple_of(j * cap, cap), cap)
            remote(
                send.at[k, c, block], recv.at[k, c, block], d_send.at[k, c], d_recv.at[k, c],
                {"ep": member(j)},
            ).start()

    def give_back(k, c):
        @pl.loop(1, half)
        def _(j):
            block = pl.ds(pl.multiple_of(j * cap, cap), cap)
            remote(
                res.at[k, c, block], ret.at[k, c, block], r_send.at[k, c], r_recv.at[k, c],
                {"ep": member(half - j)},
            ).start()

    place(0, meta_ref[...])
    squares = jnp.zeros((tokens, 1), jnp.float32)
    for c in range(CHUNKS):
        xs = x_ref[:, c * cw : (c + 1) * cw].astype(jnp.float32)
        squares = squares + jnp.sum(xs * xs, axis=-1, keepdims=True)
    scale = lax.rsqrt(squares / width + EPSILON)
    proxied = []
    for c in range(CHUNKS):
        xs = x_ref[:, c * cw : (c + 1) * cw].astype(jnp.float32)
        normed[c] = (xs * scale * pre_ref[:, c * cw : (c + 1) * cw]).astype(jnp.bfloat16)
        copy = remote(normed.at[c], prox.at[c], p_send.at[c], p_recv.at[c], {"ep": proxy})
        copy.start()
        proxied.append(copy)
        dispatch(0, c, normed[c])

    meta_copy = remote(meta_ref, pmeta, m_send, m_recv, {"ep": proxy})
    meta_copy.wait_recv()
    place(1, pmeta[...])

    def relay(c):
        proxied[c].wait_recv()
        dispatch(1, c, prox[c])

    def received(k):
        for c in range(CHUNKS):
            await_bytes(recv.at[k, c, pl.ds(cap, rows - cap)], d_recv.at[k, c])

    def expand(k):
        for h in range(tps):
            @pl.loop(0, fh // TILE)
            def _(t):
                at = pl.ds(pl.multiple_of(t * TILE, TILE), TILE)
                gate = jnp.zeros((rows, TILE), jnp.float32)
                up = jnp.zeros((rows, TILE), jnp.float32)
                for c in range(CHUNKS):
                    gate += dot(recv[k, c], gate_v[h, c * cw : (c + 1) * cw, at])
                    up += dot(recv[k, c], up_v[h, c * cw : (c + 1) * cw, at])
                hidden[h, :, at] = activate(gate, up)

    def contract(k, c):
        for t in range(cw // TILE):
            lo = t * TILE
            total = jnp.zeros((rows, TILE), jnp.float32)
            for h in range(tps):
                at = pl.ds(pl.multiple_of(c * cw + lo, TILE), TILE)
                total += dot(hidden[h], down_v[h, :, at]).astype(jnp.bfloat16).astype(jnp.float32)
            total = total.astype(jnp.bfloat16)
            ret[k, c, 0:cap, lo : lo + TILE] = total[0:cap]
            res[k, c, cap:rows, lo : lo + TILE] = total[cap:rows]
        give_back(k, c)

    relay(0)
    relay(1)
    for copy in local_copies:
        copy.wait()
    for copy in peer_copies:
        copy.wait()
    received(0)
    expand(0)
    relay(2)

    @pl.loop(0, CHUNKS)
    def _(c):
        contract(0, c)

    relay(3)
    received(1)
    expand(1)

    @pl.loop(0, CHUNKS)
    def _(c):
        contract(1, c)

    high0, low0 = mixer(0)
    for c in range(CHUNKS):
        await_bytes(ret.at[0, c, pl.ds(cap, rows - cap)], r_recv.at[0, c])
        mixed[c] = dot(high0, ret[0, c]) + dot(low0, ret[0, c])
    high1, low1 = mixer(1)
    shares = []
    for c in range(CHUNKS):
        await_bytes(ret.at[1, c, pl.ds(cap, rows - cap)], r_recv.at[1, c])
        part_send[c] = (dot(high1, ret[1, c]) + dot(low1, ret[1, c])).astype(jnp.bfloat16)
        copy = remote(part_send.at[c], part_recv.at[c], q_send.at[c], q_recv.at[c], {"ep": proxy})
        copy.start()
        shares.append(copy)

    squares = jnp.zeros((tokens, 1), jnp.float32)
    for c in range(CHUNKS):
        shares[c].wait_recv()
        total = mixed[c] + part_recv[c].astype(jnp.float32)
        mixed[c] = total
        squares = squares + jnp.sum(total * total, axis=-1, keepdims=True)
    scale = lax.rsqrt(squares / width + EPSILON)
    for c in range(CHUNKS):
        at = slice(c * cw, (c + 1) * cw)
        out_ref[:, at] = (mixed[c] * scale * post_ref[:, at]).astype(jnp.bfloat16)

    meta_copy.wait_send()
    for c in range(CHUNKS):
        proxied[c].wait_send()
        shares[c].wait_send()
        for k in range(2):
            await_bytes(send.at[k, c, pl.ds(cap, rows - cap)], d_send.at[k, c])
            await_bytes(res.at[k, c, pl.ds(cap, rows - cap)], r_send.at[k, c])


def local(inputs, pre_gain, expert_ids, route_weights, gate_proj, up_proj, down_proj, post_gain):
    tokens, width = inputs.shape
    choices = expert_ids.shape[1]
    n = lax.axis_size("ep")
    tps = lax.axis_size("tp")
    cap = 3 * tokens * choices // (2 * n * gate_proj.shape[0])
    cap = -(-cap // 16) * 16
    half = n // 2
    rows = half * cap
    cw = width // CHUNKS
    fh = gate_proj.shape[2]
    meta = jnp.concatenate(
        [
            expert_ids.astype(jnp.float32),
            route_weights,
            jnp.zeros((tokens, 8 - 2 * choices), jnp.float32),
        ],
        axis=1,
    ).T
    bf16 = jnp.bfloat16
    vmem = pl.BlockSpec(memory_space=pltpu.VMEM)
    hbm = pl.BlockSpec(memory_space=pl.ANY)
    dma = pltpu.SemaphoreType.DMA
    return pl.pallas_call(
        functools.partial(kernel, n, tps, cap),
        out_shape=jax.ShapeDtypeStruct((tokens, width), bf16),
        in_specs=[vmem, vmem, vmem, hbm, hbm, hbm, vmem],
        out_specs=vmem,
        scratch_shapes=[
            pltpu.VMEM((tps, width, fh), bf16),
            pltpu.VMEM((tps, width, fh), bf16),
            pltpu.VMEM((tps, fh, width), bf16),
            pltpu.VMEM((CHUNKS, tokens, cw), bf16),
            pltpu.VMEM((CHUNKS, tokens, cw), bf16),
            pltpu.VMEM((8, tokens), jnp.float32),
            pltpu.VMEM((2, CHUNKS, rows, cw), bf16),
            pltpu.VMEM((2, CHUNKS, rows, cw), bf16),
            pltpu.VMEM((2, CHUNKS, rows, cw), bf16),
            pltpu.VMEM((2, CHUNKS, rows, cw), bf16),
            pltpu.VMEM((CHUNKS, tokens, cw), bf16),
            pltpu.VMEM((CHUNKS, tokens, cw), bf16),
            pltpu.VMEM((CHUNKS, tokens, cw), jnp.float32),
            pltpu.VMEM((tps, rows, fh), bf16),
            pltpu.VMEM((2, 8, tokens), jnp.float32),
            dma((3,)), dma((3, tps - 1)), dma((3, tps - 1)),
            dma((CHUNKS,)), dma((CHUNKS,)), dma, dma,
            dma((2, CHUNKS)), dma((2, CHUNKS)), dma((2, CHUNKS)), dma((2, CHUNKS)),
            dma((CHUNKS,)), dma((CHUNKS,)),
        ],
        compiler_params=pltpu.CompilerParams(
            collective_id=0, has_side_effects=True, vmem_limit_bytes=67043328
        ),
    )(inputs, pre_gain[None, :], meta, gate_proj, up_proj, down_proj, post_gain[None, :])


def solution(mesh):
    in_specs = (
        P(("ep", "tp"), None),
        P(),
        P(("ep", "tp"), None),
        P(("ep", "tp"), None),
        P("ep", None, "tp"),
        P("ep", None, "tp"),
        P("ep", "tp", None),
        P(),
    )
    out_specs = P(("ep", "tp"), None)
    return jax.shard_map(local, mesh=mesh, in_specs=in_specs, out_specs=out_specs, check_vma=False)
```

```python
import functools

import jax
import jax.numpy as jnp
from jax import lax
from jax.experimental import pallas as pl
from jax.experimental.pallas import tpu as pltpu
from jax.sharding import PartitionSpec as P

EPSILON = 1e-06
LIMIT = 7.0
ALPHA = 1.702
CHUNKS = 4
TILE = 256
MESH = pl.DeviceIdType.MESH


def activate(gate, up):
    gate = jnp.minimum(gate, LIMIT)
    up = jnp.clip(up, -LIMIT, LIMIT)
    return ((up + 1.0) * gate * jax.nn.sigmoid(ALPHA * gate)).astype(jnp.bfloat16)


def dot(a, b):
    return jnp.dot(a, b, preferred_element_type=jnp.float32)


def kernel(
    n, tps, cap,
    x_ref, pre_ref, meta_ref, gate_ref, up_ref, down_ref, post_ref, out_ref,
    gate_v, up_v, down_v, normed, prox, pmeta, send, recv, ret, acc, part_send, part_recv,
    mixed, hidden, places,
    w_local, w_send, w_recv, p_send, p_recv, m_send, m_recv,
    d_send, d_recv, r_send, r_recv, q_send, q_recv,
):
    half = n // 2
    tokens, width = x_ref.shape
    cw = width // CHUNKS
    rows = half * cap
    fh = gate_v.shape[2]
    me = lax.axis_index("ep")
    core = lax.axis_index("tp")
    base = (me // half) * half
    mine = lax.rem(me, half)
    proxy = lax.rem(me + half, n)

    def member(j):
        return base + lax.rem(mine + j, half)

    barrier = pltpu.get_barrier_semaphore()

    @pl.loop(1, half)
    def _(j):
        pl.semaphore_signal(barrier, inc=1, device_id={"ep": member(j)}, device_id_type=MESH)

    pl.semaphore_signal(barrier, inc=1, device_id={"ep": proxy}, device_id_type=MESH)
    for i in range(1, tps):
        pl.semaphore_signal(
            barrier, inc=1, device_id={"tp": lax.rem(core + i, tps)}, device_id_type=MESH
        )
    pl.semaphore_wait(barrier, half + tps - 1)

    def remote(src, dst, ss, rs, where):
        return pltpu.make_async_remote_copy(
            src_ref=src, dst_ref=dst, send_sem=ss, recv_sem=rs,
            device_id=where, device_id_type=MESH,
        )

    def await_bytes(ref, sem):
        pltpu.make_async_copy(ref, ref, sem).wait()

    remote(meta_ref, pmeta, m_send, m_recv, {"ep": proxy}).start()
    weights = ((gate_ref, gate_v), (up_ref, up_v), (down_ref, down_v))
    local_copies, peer_copies = [], []
    for w, (src, dst) in enumerate(weights):
        local_copies.append(pltpu.make_async_copy(src.at[0], dst.at[core], w_local.at[w]))
        for i in range(1, tps):
            peer_copies.append(
                remote(
                    src.at[0], dst.at[core], w_send.at[w, i - 1], w_recv.at[w, i - 1],
                    {"tp": lax.rem(core + i, tps)},
                )
            )
    for copy in peer_copies + local_copies:
        copy.start()

    experts_col = lax.broadcasted_iota(jnp.int32, (n, 1), 0).astype(jnp.float32)
    earlier_mask = (
        lax.broadcasted_iota(jnp.int32, (tokens, tokens), 0)
        < lax.broadcasted_iota(jnp.int32, (tokens, tokens), 1)
    ).astype(jnp.bfloat16)

    def place(k, meta):
        first, second = meta[0:1, :], meta[1:2, :]
        hot0 = (first == experts_col).astype(jnp.float32)
        hot1 = (second == experts_col).astype(jnp.float32)
        before = dot((hot0 + hot1).astype(jnp.bfloat16), earlier_mask)
        places[k] = meta
        for i, (ids, hot) in enumerate(((first, hot0), (second, hot1))):
            slot = jnp.sum(before * hot, axis=0, keepdims=True)
            relative = ids - (base + mine).astype(jnp.float32)
            inside = (ids >= base.astype(jnp.float32)) & (
                ids < (base + half).astype(jnp.float32)
            )
            relative = jnp.where(relative < 0, relative + half, relative)
            places[k, i : i + 1, :] = jnp.where(inside, relative * cap + slot, -1.0)

    def picker(k):
        at = lax.broadcasted_iota(jnp.int32, (rows, 1), 0).astype(jnp.float32)
        return (
            (places[k, 0:1, :] == at).astype(jnp.float32)
            + (places[k, 1:2, :] == at).astype(jnp.float32)
        ).astype(jnp.bfloat16)

    def mixer(k):
        columns = places[k].T
        at = lax.broadcasted_iota(jnp.int32, (1, rows), 1).astype(jnp.float32)
        w = jnp.where(columns[:, 0:1] == at, columns[:, 2:3], 0.0) + jnp.where(
            columns[:, 1:2] == at, columns[:, 3:4], 0.0
        )
        high = w.astype(jnp.bfloat16)
        return high, (w - high.astype(jnp.float32)).astype(jnp.bfloat16)

    def dispatch(k, c, values):
        picked = dot(picker(k), values).astype(jnp.bfloat16)
        recv[k, c, 0:cap, :] = picked[0:cap]
        send[k, c, cap:rows, :] = picked[cap:rows]

        @pl.loop(1, half)
        def _(j):
            block = pl.ds(pl.multiple_of(j * cap, cap), cap)
            remote(
                send.at[k, c, block], recv.at[k, c, block], d_send.at[k, c], d_recv.at[k, c],
                {"ep": member(j)},
            ).start()

    def give_back(k, c):
        @pl.loop(1, half)
        def _(j):
            block = pl.ds(pl.multiple_of(j * cap, cap), cap)
            remote(
                send.at[k, c, block], ret.at[k, c, block], r_send.at[k, c], r_recv.at[k, c],
                {"ep": member(half - j)},
            ).start()

    squares = jnp.zeros((tokens, 1), jnp.float32)
    for c in range(CHUNKS):
        xs = x_ref[:, c * cw : (c + 1) * cw].astype(jnp.float32)
        squares = squares + jnp.sum(xs * xs, axis=-1, keepdims=True)
    scale = lax.rsqrt(squares / width + EPSILON)
    proxied = [
        remote(normed.at[c], prox.at[c], p_send.at[c], p_recv.at[c], {"ep": proxy})
        for c in range(CHUNKS)
    ]

    def normalise(c):
        xs = x_ref[:, c * cw : (c + 1) * cw].astype(jnp.float32)
        normed[c] = (xs * scale * pre_ref[:, c * cw : (c + 1) * cw]).astype(jnp.bfloat16)

    def own(c):
        dispatch(0, c, normed[c])

    def relay(c):
        proxied[c].wait_recv()
        dispatch(1, c, prox[c])

    meta_copy = remote(meta_ref, pmeta, m_send, m_recv, {"ep": proxy})
    normalise(0)
    proxied[0].start()
    place(0, meta_ref[...])
    own(0)
    normalise(1)
    proxied[1].start()
    own(1)
    normalise(2)
    normalise(3)
    meta_copy.wait_recv()
    place(1, pmeta[...])

    def received(k, c):
        await_bytes(recv.at[k, c, pl.ds(cap, rows - cap)], d_recv.at[k, c])

    def expand(k, halves, chunks, begin=True, end=True, tiles=(0, fh // TILE)):
        for h in halves:
            @pl.loop(*tiles)
            def _(t):
                at = pl.ds(pl.multiple_of(t * TILE, TILE), TILE)
                if begin:
                    gate = jnp.zeros((rows, TILE), jnp.float32)
                    up = jnp.zeros((rows, TILE), jnp.float32)
                else:
                    gate = acc[0, h, :, at]
                    up = acc[1, h, :, at]
                for c in chunks:
                    gate += dot(recv[k, c], gate_v[h, c * cw : (c + 1) * cw, at])
                    up += dot(recv[k, c], up_v[h, c * cw : (c + 1) * cw, at])
                if end:
                    hidden[k, h, :, at] = activate(gate, up)
                else:
                    acc[0, h, :, at] = gate
                    acc[1, h, :, at] = up

    def contract(k, c):
        await_bytes(send.at[k, c, pl.ds(cap, rows - cap)], d_send.at[k, c])
        for t in range(cw // TILE):
            lo = t * TILE
            total = jnp.zeros((rows, TILE), jnp.float32)
            for h in range(tps):
                at = pl.ds(pl.multiple_of(c * cw + lo, TILE), TILE)
                total += dot(hidden[k, h], down_v[h, :, at]).astype(jnp.bfloat16).astype(jnp.float32)
            total = total.astype(jnp.bfloat16)
            ret[k, c, 0:cap, lo : lo + TILE] = total[0:cap]
            send[k, c, cap:rows, lo : lo + TILE] = total[cap:rows]
        give_back(k, c)

    both = range(tps)
    last = fh // TILE
    relay(0)
    proxied[2].start()
    for copy in local_copies:
        copy.wait()
    for copy in peer_copies:
        copy.wait()
    relay(1)
    proxied[3].start()
    received(1, 0)
    received(1, 1)
    expand(1, both, (0, 1), end=False)
    relay(2)
    received(1, 2)
    expand(1, both, (2,), begin=False, end=False)
    relay(3)
    own(2)
    own(3)
    received(1, 3)
    expand(1, both, (3,), begin=False)

    shares = []
    high1, low1 = mixer(1)

    def share(c):
        await_bytes(ret.at[1, c, pl.ds(cap, rows - cap)], r_recv.at[1, c])
        part_send[c] = (dot(high1, ret[1, c]) + dot(low1, ret[1, c])).astype(jnp.bfloat16)
        copy = remote(part_send.at[c], part_recv.at[c], q_send.at[c], q_recv.at[c], {"ep": proxy})
        copy.start()
        shares.append(copy)

    contract(1, 0)
    contract(1, 1)
    for c in range(CHUNKS):
        received(0, c)
    every = range(CHUNKS)
    expand(0, (0,), every, tiles=(0, last // 2))
    share(0)
    contract(1, 2)
    expand(0, (0,), every, tiles=(last // 2, last))
    share(1)
    contract(1, 3)
    expand(0, range(1, tps), every, tiles=(0, last // 2))
    share(2)
    expand(0, range(1, tps), every, tiles=(last // 2, last))
    share(3)

    @pl.loop(0, CHUNKS)
    def _(c):
        contract(0, c)

    high0, low0 = mixer(0)
    for c in range(CHUNKS):
        await_bytes(ret.at[0, c, pl.ds(cap, rows - cap)], r_recv.at[0, c])
        mixed[c] = dot(high0, ret[0, c]) + dot(low0, ret[0, c])

    squares = jnp.zeros((tokens, 1), jnp.float32)
    for c in range(CHUNKS):
        shares[c].wait_recv()
        total = mixed[c] + part_recv[c].astype(jnp.float32)
        mixed[c] = total
        squares = squares + jnp.sum(total * total, axis=-1, keepdims=True)
    scale = lax.rsqrt(squares / width + EPSILON)
    for c in range(CHUNKS):
        at = slice(c * cw, (c + 1) * cw)
        out_ref[:, at] = (mixed[c] * scale * post_ref[:, at]).astype(jnp.bfloat16)

    meta_copy.wait_send()
    for c in range(CHUNKS):
        proxied[c].wait_send()
        shares[c].wait_send()
        for k in range(2):
            await_bytes(send.at[k, c, pl.ds(cap, rows - cap)], r_send.at[k, c])


def local(inputs, pre_gain, expert_ids, route_weights, gate_proj, up_proj, down_proj, post_gain):
    tokens, width = inputs.shape
    choices = expert_ids.shape[1]
    n = lax.axis_size("ep")
    tps = lax.axis_size("tp")
    cap = 3 * tokens * choices // (2 * n * gate_proj.shape[0])
    cap = -(-cap // 16) * 16
    half = n // 2
    rows = half * cap
    cw = width // CHUNKS
    fh = gate_proj.shape[2]
    meta = jnp.concatenate(
        [
            expert_ids.astype(jnp.float32),
            route_weights,
            jnp.zeros((tokens, 8 - 2 * choices), jnp.float32),
        ],
        axis=1,
    ).T
    bf16 = jnp.bfloat16
    vmem = pl.BlockSpec(memory_space=pltpu.VMEM)
    hbm = pl.BlockSpec(memory_space=pl.ANY)
    dma = pltpu.SemaphoreType.DMA
    return pl.pallas_call(
        functools.partial(kernel, n, tps, cap),
        out_shape=jax.ShapeDtypeStruct((tokens, width), bf16),
        in_specs=[vmem, vmem, vmem, hbm, hbm, hbm, vmem],
        out_specs=vmem,
        scratch_shapes=[
            pltpu.VMEM((tps, width, fh), bf16),
            pltpu.VMEM((tps, width, fh), bf16),
            pltpu.VMEM((tps, fh, width), bf16),
            pltpu.VMEM((CHUNKS, tokens, cw), bf16),
            pltpu.VMEM((CHUNKS, tokens, cw), bf16),
            pltpu.VMEM((8, tokens), jnp.float32),
            pltpu.VMEM((2, CHUNKS, rows, cw), bf16),
            pltpu.VMEM((2, CHUNKS, rows, cw), bf16),
            pltpu.VMEM((2, CHUNKS, rows, cw), bf16),
            pltpu.VMEM((2, tps, rows, fh), jnp.float32),
            pltpu.VMEM((CHUNKS, tokens, cw), bf16),
            pltpu.VMEM((CHUNKS, tokens, cw), bf16),
            pltpu.VMEM((CHUNKS, tokens, cw), jnp.float32),
            pltpu.VMEM((2, tps, rows, fh), bf16),
            pltpu.VMEM((2, 8, tokens), jnp.float32),
            dma((3,)), dma((3, tps - 1)), dma((3, tps - 1)),
            dma((CHUNKS,)), dma((CHUNKS,)), dma, dma,
            dma((2, CHUNKS)), dma((2, CHUNKS)), dma((2, CHUNKS)), dma((2, CHUNKS)),
            dma((CHUNKS,)), dma((CHUNKS,)),
        ],
        compiler_params=pltpu.CompilerParams(
            collective_id=0, has_side_effects=True, vmem_limit_bytes=67043328
        ),
    )(inputs, pre_gain[None, :], meta, gate_proj, up_proj, down_proj, post_gain[None, :])


def solution(mesh):
    in_specs = (
        P(("ep", "tp"), None),
        P(),
        P(("ep", "tp"), None),
        P(("ep", "tp"), None),
        P("ep", None, "tp"),
        P("ep", None, "tp"),
        P("ep", "tp", None),
        P(),
    )
    out_specs = P(("ep", "tp"), None)
    return jax.shard_map(local, mesh=mesh, in_specs=in_specs, out_specs=out_specs, check_vma=False)
```

```python
import functools

import jax
import jax.numpy as jnp
from jax import lax
from jax.experimental import pallas as pl
from jax.experimental.pallas import tpu as pltpu
from jax.sharding import PartitionSpec as P

EPSILON = 1e-06
LIMIT = 7.0
ALPHA = 1.702
CHUNKS = 4
TILE = 256
MESH = pl.DeviceIdType.MESH


def activate(gate, up):
    gate = jnp.minimum(gate, LIMIT)
    up = jnp.clip(up, -LIMIT, LIMIT)
    return ((up + 1.0) * gate * jax.nn.sigmoid(ALPHA * gate)).astype(jnp.bfloat16)


def dot(a, b):
    return jnp.dot(a, b, preferred_element_type=jnp.float32)


def kernel(
    n, tps, cap,
    x_ref, pre_ref, meta_ref, gate_ref, up_ref, down_ref, post_ref, out_ref,
    gate_v, up_v, down_v, normed, prox, pmeta, send, recv, ret, acc, part_send, part_recv,
    mixed, hidden, places,
    w_local, w_send, w_recv, p_send, p_recv, m_send, m_recv,
    d_send, d_recv, r_send, r_recv, q_send, q_recv,
):
    half = n // 2
    tokens, width = x_ref.shape
    cw = width // CHUNKS
    rows = half * cap
    fh = gate_v.shape[2]
    me = lax.axis_index("ep")
    core = lax.axis_index("tp")
    base = (me // half) * half
    mine = lax.rem(me, half)
    proxy = lax.rem(me + half, n)

    def member(j):
        return base + lax.rem(mine + j, half)

    barrier = pltpu.get_barrier_semaphore()

    @pl.loop(1, half)
    def _(j):
        pl.semaphore_signal(barrier, inc=1, device_id={"ep": member(j)}, device_id_type=MESH)

    pl.semaphore_signal(barrier, inc=1, device_id={"ep": proxy}, device_id_type=MESH)
    for i in range(1, tps):
        pl.semaphore_signal(
            barrier, inc=1, device_id={"tp": lax.rem(core + i, tps)}, device_id_type=MESH
        )
    pl.semaphore_wait(barrier, half + tps - 1)

    def remote(src, dst, ss, rs, where):
        return pltpu.make_async_remote_copy(
            src_ref=src, dst_ref=dst, send_sem=ss, recv_sem=rs,
            device_id=where, device_id_type=MESH,
        )

    def await_bytes(ref, sem):
        pltpu.make_async_copy(ref, ref, sem).wait()

    remote(meta_ref, pmeta, m_send, m_recv, {"ep": proxy}).start()
    weights = ((gate_ref, gate_v), (up_ref, up_v), (down_ref, down_v))
    local_copies, peer_copies = [], []
    for w, (src, dst) in enumerate(weights):
        local_copies.append(pltpu.make_async_copy(src.at[0], dst.at[core], w_local.at[w]))
        for i in range(1, tps):
            peer_copies.append(
                remote(
                    src.at[0], dst.at[core], w_send.at[w, i - 1], w_recv.at[w, i - 1],
                    {"tp": lax.rem(core + i, tps)},
                )
            )
    for copy in peer_copies + local_copies:
        copy.start()

    experts_col = lax.broadcasted_iota(jnp.int32, (n, 1), 0).astype(jnp.float32)
    earlier_mask = (
        lax.broadcasted_iota(jnp.int32, (tokens, tokens), 0)
        < lax.broadcasted_iota(jnp.int32, (tokens, tokens), 1)
    ).astype(jnp.bfloat16)

    def place(k, meta):
        first, second = meta[0:1, :], meta[1:2, :]
        hot0 = (first == experts_col).astype(jnp.float32)
        hot1 = (second == experts_col).astype(jnp.float32)
        before = dot((hot0 + hot1).astype(jnp.bfloat16), earlier_mask)
        places[k] = meta
        for i, (ids, hot) in enumerate(((first, hot0), (second, hot1))):
            slot = jnp.sum(before * hot, axis=0, keepdims=True)
            relative = ids - (base + mine).astype(jnp.float32)
            inside = (ids >= base.astype(jnp.float32)) & (
                ids < (base + half).astype(jnp.float32)
            )
            relative = jnp.where(relative < 0, relative + half, relative)
            places[k, i : i + 1, :] = jnp.where(inside, relative * cap + slot, -1.0)

    def picker(k):
        at = lax.broadcasted_iota(jnp.int32, (rows, 1), 0).astype(jnp.float32)
        return (
            (places[k, 0:1, :] == at).astype(jnp.float32)
            + (places[k, 1:2, :] == at).astype(jnp.float32)
        ).astype(jnp.bfloat16)

    def mixer(k):
        columns = places[k].T
        at = lax.broadcasted_iota(jnp.int32, (1, rows), 1).astype(jnp.float32)
        w = jnp.where(columns[:, 0:1] == at, columns[:, 2:3], 0.0) + jnp.where(
            columns[:, 1:2] == at, columns[:, 3:4], 0.0
        )
        high = w.astype(jnp.bfloat16)
        return high, (w - high.astype(jnp.float32)).astype(jnp.bfloat16)

    def dispatch(k, c, values):
        picked = dot(picker(k), values).astype(jnp.bfloat16)
        recv[k, c, 0:cap, :] = picked[0:cap]
        send[k, c, cap:rows, :] = picked[cap:rows]

        @pl.loop(1, half)
        def _(j):
            block = pl.ds(pl.multiple_of(j * cap, cap), cap)
            remote(
                send.at[k, c, block], recv.at[k, c, block], d_send.at[k, c], d_recv.at[k, c],
                {"ep": member(j)},
            ).start()

    def give_back(k, c):
        @pl.loop(1, half)
        def _(j):
            block = pl.ds(pl.multiple_of(j * cap, cap), cap)
            remote(
                send.at[k, c, block], ret.at[k, c, block], r_send.at[k, c], r_recv.at[k, c],
                {"ep": member(half - j)},
            ).start()

    squares = jnp.zeros((tokens, 1), jnp.float32)
    for c in range(CHUNKS):
        xs = x_ref[:, c * cw : (c + 1) * cw].astype(jnp.float32)
        squares = squares + jnp.sum(xs * xs, axis=-1, keepdims=True)
    scale = lax.rsqrt(squares / width + EPSILON)
    proxied = [
        remote(normed.at[c], prox.at[c], p_send.at[c], p_recv.at[c], {"ep": proxy})
        for c in range(CHUNKS)
    ]

    def normalise(c):
        xs = x_ref[:, c * cw : (c + 1) * cw].astype(jnp.float32)
        normed[c] = (xs * scale * pre_ref[:, c * cw : (c + 1) * cw]).astype(jnp.bfloat16)

    def own(c):
        dispatch(0, c, normed[c])

    def relay(c):
        proxied[c].wait_recv()
        dispatch(1, c, prox[c])

    meta_copy = remote(meta_ref, pmeta, m_send, m_recv, {"ep": proxy})
    normalise(0)
    proxied[0].start()
    place(0, meta_ref[...])
    own(0)
    normalise(1)
    proxied[1].start()
    own(1)
    normalise(2)
    proxied[2].start()
    own(2)
    normalise(3)
    proxied[3].start()
    own(3)
    meta_copy.wait_recv()
    place(1, pmeta[...])

    def received(k, c):
        await_bytes(recv.at[k, c, pl.ds(cap, rows - cap)], d_recv.at[k, c])

    def expand(k, halves, chunks, begin=True, end=True, tiles=(0, fh // TILE)):
        for h in halves:
            @pl.loop(*tiles)
            def _(t):
                at = pl.ds(pl.multiple_of(t * TILE, TILE), TILE)
                if begin:
                    gate = jnp.zeros((rows, TILE), jnp.float32)
                    up = jnp.zeros((rows, TILE), jnp.float32)
                else:
                    gate = acc[0, h, :, at]
                    up = acc[1, h, :, at]
                for c in chunks:
                    gate += dot(recv[k, c], gate_v[h, c * cw : (c + 1) * cw, at])
                    up += dot(recv[k, c], up_v[h, c * cw : (c + 1) * cw, at])
                if end:
                    hidden[k, h, :, at] = activate(gate, up)
                else:
                    acc[0, h, :, at] = gate
                    acc[1, h, :, at] = up

    def contract(k, c):
        await_bytes(send.at[k, c, pl.ds(cap, rows - cap)], d_send.at[k, c])
        for t in range(cw // TILE):
            lo = t * TILE
            total = jnp.zeros((rows, TILE), jnp.float32)
            for h in range(tps):
                at = pl.ds(pl.multiple_of(c * cw + lo, TILE), TILE)
                total += dot(hidden[k, h], down_v[h, :, at]).astype(jnp.bfloat16).astype(jnp.float32)
            total = total.astype(jnp.bfloat16)
            ret[k, c, 0:cap, lo : lo + TILE] = total[0:cap]
            send[k, c, cap:rows, lo : lo + TILE] = total[cap:rows]
        give_back(k, c)

    both = range(tps)
    last = fh // TILE
    relay(0)
    for copy in local_copies:
        copy.wait()
    for copy in peer_copies:
        copy.wait()
    relay(1)
    received(1, 0)
    received(1, 1)
    expand(1, both, (0, 1), end=False)
    relay(2)
    received(1, 2)
    expand(1, both, (2,), begin=False, end=False)
    relay(3)
    received(1, 3)
    expand(1, both, (3,), begin=False)

    shares = []
    high1, low1 = mixer(1)

    def share(c):
        await_bytes(ret.at[1, c, pl.ds(cap, rows - cap)], r_recv.at[1, c])
        part_send[c] = (dot(high1, ret[1, c]) + dot(low1, ret[1, c])).astype(jnp.bfloat16)
        copy = remote(part_send.at[c], part_recv.at[c], q_send.at[c], q_recv.at[c], {"ep": proxy})
        copy.start()
        shares.append(copy)

    contract(1, 0)
    contract(1, 1)
    for c in range(CHUNKS):
        received(0, c)
    every = range(CHUNKS)
    expand(0, (0,), every, tiles=(0, last // 2))
    share(0)
    contract(1, 2)
    expand(0, (0,), every, tiles=(last // 2, last))
    share(1)
    contract(1, 3)
    expand(0, range(1, tps), every, tiles=(0, last // 2))
    share(2)
    expand(0, range(1, tps), every, tiles=(last // 2, last))
    share(3)

    @pl.loop(0, CHUNKS)
    def _(c):
        contract(0, c)

    high0, low0 = mixer(0)
    for c in range(CHUNKS):
        await_bytes(ret.at[0, c, pl.ds(cap, rows - cap)], r_recv.at[0, c])
        mixed[c] = dot(high0, ret[0, c]) + dot(low0, ret[0, c])

    squares = jnp.zeros((tokens, 1), jnp.float32)
    for c in range(CHUNKS):
        shares[c].wait_recv()
        total = mixed[c] + part_recv[c].astype(jnp.float32)
        mixed[c] = total
        squares = squares + jnp.sum(total * total, axis=-1, keepdims=True)
    scale = lax.rsqrt(squares / width + EPSILON)
    for c in range(CHUNKS):
        at = slice(c * cw, (c + 1) * cw)
        out_ref[:, at] = (mixed[c] * scale * post_ref[:, at]).astype(jnp.bfloat16)

    meta_copy.wait_send()
    for c in range(CHUNKS):
        proxied[c].wait_send()
        shares[c].wait_send()
        for k in range(2):
            await_bytes(send.at[k, c, pl.ds(cap, rows - cap)], r_send.at[k, c])


def local(inputs, pre_gain, expert_ids, route_weights, gate_proj, up_proj, down_proj, post_gain):
    tokens, width = inputs.shape
    choices = expert_ids.shape[1]
    n = lax.axis_size("ep")
    tps = lax.axis_size("tp")
    cap = 3 * tokens * choices // (2 * n * gate_proj.shape[0])
    cap = -(-cap // 16) * 16
    half = n // 2
    rows = half * cap
    cw = width // CHUNKS
    fh = gate_proj.shape[2]
    meta = jnp.concatenate(
        [
            expert_ids.astype(jnp.float32),
            route_weights,
            jnp.zeros((tokens, 8 - 2 * choices), jnp.float32),
        ],
        axis=1,
    ).T
    bf16 = jnp.bfloat16
    vmem = pl.BlockSpec(memory_space=pltpu.VMEM)
    hbm = pl.BlockSpec(memory_space=pl.ANY)
    dma = pltpu.SemaphoreType.DMA
    return pl.pallas_call(
        functools.partial(kernel, n, tps, cap),
        out_shape=jax.ShapeDtypeStruct((tokens, width), bf16),
        in_specs=[vmem, vmem, vmem, hbm, hbm, hbm, vmem],
        out_specs=vmem,
        scratch_shapes=[
            pltpu.VMEM((tps, width, fh), bf16),
            pltpu.VMEM((tps, width, fh), bf16),
            pltpu.VMEM((tps, fh, width), bf16),
            pltpu.VMEM((CHUNKS, tokens, cw), bf16),
            pltpu.VMEM((CHUNKS, tokens, cw), bf16),
            pltpu.VMEM((8, tokens), jnp.float32),
            pltpu.VMEM((2, CHUNKS, rows, cw), bf16),
            pltpu.VMEM((2, CHUNKS, rows, cw), bf16),
            pltpu.VMEM((2, CHUNKS, rows, cw), bf16),
            pltpu.VMEM((2, tps, rows, fh), jnp.float32),
            pltpu.VMEM((CHUNKS, tokens, cw), bf16),
            pltpu.VMEM((CHUNKS, tokens, cw), bf16),
            pltpu.VMEM((CHUNKS, tokens, cw), jnp.float32),
            pltpu.VMEM((2, tps, rows, fh), bf16),
            pltpu.VMEM((2, 8, tokens), jnp.float32),
            dma((3,)), dma((3, tps - 1)), dma((3, tps - 1)),
            dma((CHUNKS,)), dma((CHUNKS,)), dma, dma,
            dma((2, CHUNKS)), dma((2, CHUNKS)), dma((2, CHUNKS)), dma((2, CHUNKS)),
            dma((CHUNKS,)), dma((CHUNKS,)),
        ],
        compiler_params=pltpu.CompilerParams(
            collective_id=0, has_side_effects=True, vmem_limit_bytes=67043328
        ),
    )(inputs, pre_gain[None, :], meta, gate_proj, up_proj, down_proj, post_gain[None, :])


def solution(mesh):
    in_specs = (
        P(("ep", "tp"), None),
        P(),
        P(("ep", "tp"), None),
        P(("ep", "tp"), None),
        P("ep", None, "tp"),
        P("ep", None, "tp"),
        P("ep", "tp", None),
        P(),
    )
    out_specs = P(("ep", "tp"), None)
    return jax.shard_map(local, mesh=mesh, in_specs=in_specs, out_specs=out_specs, check_vma=False)
```
